128 devices in a mesh: ep: 64 (over z, y, x), tp: 2 (over core).
Axes of the slice: x: 4, y: 4, z: 4, core: 2. Of those that a mesh axis runs over, the one named last changes fastest.
Arguments:
- inputs: bfloat16 [32768, 2048], P(('ep', 'tp')), may hold values from -6 to 6
- pre_gain: float32 [2048], replicated, may hold values from 0.5 to 8
- expert_ids: int32 [32768, 2], P(('ep', 'tp')), may hold values from 0 to 63, all different within a row; in each aligned block of 256 rows (0 to 255, 256 to 511, ...) at most 12 rows name the same one
- route_weights: float32 [32768, 2], P(('ep', 'tp')), may hold values from 0.05 to 1
- gate_proj: bfloat16 [64, 2048, 2048], P('ep', None, 'tp'), may hold values from -0.125 to 0.125
- up_proj: bfloat16 [64, 2048, 2048], P('ep', None, 'tp'), may hold values from -0.125 to 0.125
- down_proj: bfloat16 [64, 2048, 2048], P('ep', 'tp'), may hold values from -0.125 to 0.125
- post_gain: float32 [2048], replicated, may hold values from 0.1 to 1.9
Outputs:
- layer_out: bfloat16 [32768, 2048], P(('ep', 'tp'))
The draws below stay inside these ranges and needn't reach their ends.
Inputs may be any that keep to these rules, and one draw needn't show every extreme that they name: `expert_ids`: each token names 2 different experts. Among the 256 tokens of one device (aligned blocks of rows) no expert is named by more than 12 tokens, and in every draw some expert is named by exactly 12 tokens of some device.
All inputs are finite; a program needn't handle non-finite values.
Results may differ from the reference program's by a relative error of at most 0.0095.
Values may be sent and summed in bfloat16 or wider, within the bound.
A program may use at most 128 MiB of HBM per device.

```python
import math
import jax
import jax.numpy as jnp
import numpy as np
from jax import lax

D = 2048
FE = 2048
TOP_K = 2
TOK_DEV = 256
EXPERTS = 64
CAP = 12
TOKENS = 32768
N_EP = 64
N_TP = 2


def draw_pre_gain(key, part):
    return 1.0 + 0.18 * jnp.clip(jax.random.normal(key, (D,), jnp.float32), -2.5, 2.5)


def level_of(rng, dims, split, low, high):
    loudness = 1.0
    for dim, shards_of in split:
        steps = jax.random.uniform(jax.random.fold_in(jax.random.fold_in(rng, 6), dim), (shards_of,), jnp.float32, low / len(split), high / len(split))
        loudness = loudness * jnp.repeat(jnp.exp(steps), dims[dim] // shards_of).reshape((-1,) + (1,) * (len(dims) - 1 - dim))
    return loudness


def shared_out(stream_key, own, number, rows, count, top, reach, skew):
    sequence = jax.random.permutation(stream_key, count)
    packed, ordinary = shares(count, rows * top, reach, skew, True), shares(count, rows * top, reach, skew, False)
    places = jnp.arange(count)

    def named(tallies, turn):
        used = int((tallies > 0).sum())
        fixed = max(1, used // 4)
        moved = fixed + (places - fixed + turn * (used - fixed)) % max(1, count - fixed)
        return jnp.zeros((count,), jnp.int32).at[sequence[jnp.where(places < fixed, places, moved)]].set(jnp.asarray(tallies, jnp.int32))

    tallies = jnp.where(number % 4 == 0, named(packed, number // 4), named(ordinary, number - number // 4 - 1))
    mixed = jax.random.permutation(jax.random.fold_in(own, 3), count)
    giver, taker = mixed[0:count // 2 * 2:2], mixed[1:count // 2 * 2:2]
    margin = jnp.minimum(tallies[giver] - 1, reach - tallies[taker]) // 2
    margin = jnp.where((giver == sequence[0]) | (taker == sequence[0]) | (tallies[taker] == 0), 0, jnp.maximum(margin, 0))
    moved = jax.random.randint(jax.random.fold_in(own, 4), (count // 2,), 0, 1 << 20) % (margin + 1)
    tallies = tallies.at[giver].add(-moved).at[taker].add(moved)
    items = jnp.searchsorted(jnp.cumsum(tallies), jnp.arange(rows * top), side="right").astype(jnp.int32)
    listing = items.reshape(top, rows).T
    listing = listing[jax.random.permutation(jax.random.fold_in(own, 1), rows)]
    turn = jax.random.randint(jax.random.fold_in(own, 2), (rows, 1), 0, top)
    return jnp.take_along_axis(listing, (jnp.arange(top)[None, :] + turn) % top, axis=1)


def shares(amount, total, reach, lean, full):
    portions = [(1 << 20) // math.isqrt(standing ** lean) + 1 for standing in range(1, amount + 1)]
    largest = reach if full else min(reach, max(-(-total // amount), total * portions[0] // sum(portions)))
    least = 1 if total - largest >= amount - 1 else 0
    holding, surplus = [largest] + [least] * (amount - 1), total - largest - least * (amount - 1)
    while surplus > 0:
        movable = [i for i in range(1, amount) if holding[i] < largest] or [i for i in range(1, amount) if holding[i] < reach]
        whole, left = sum([portions[i] for i in movable]), surplus
        for i in movable:
            extra = min(reach - holding[i], max(1, left * portions[i] // whole), surplus)
            holding[i] = holding[i] + extra
            surplus = surplus - extra
    return np.array(holding)


def gaussian(key, shape, scale, most, shards=(), held_as=jnp.bfloat16):
    drawn = jax.random.normal(key, shape, jnp.float32) * scale
    if len(shards) > 0:
        drawn = level_of(key, shape, shards, -0.22, 0.18) * drawn
    return jnp.clip(drawn, min=-most, max=most).astype(held_as)


def setup_inputs(seed: int = 0) -> dict:
    keys = jax.random.split(jax.random.key(seed), 9)
    inputs = gaussian(keys[0], (TOKENS, D), 1.0, 6.0, ((0, 128),))
    pre_gain = draw_pre_gain(jax.random.fold_in(keys[8], 71), 0)
    expert_ids_keys = jax.random.split(jax.random.fold_in(keys[2], 1), TOKENS // TOK_DEV)
    expert_ids_turns = jax.random.permutation(jax.random.fold_in(keys[2], 3), TOKENS // TOK_DEV)
    expert_ids = jax.vmap(lambda own, number: shared_out(jax.random.fold_in(keys[2], 2), own, number, TOK_DEV, EXPERTS, TOP_K, CAP, 2))(expert_ids_keys, expert_ids_turns).reshape((TOKENS, TOP_K))
    route_weights = jnp.clip(jnp.exp(math.log(1.0) - 2.9957323 * jax.random.uniform(keys[3], (TOKENS, TOP_K), jnp.float32) ** level_of(keys[3], (TOKENS, TOP_K), ((0, 128),), -0.2, 0.2)), 0.05, 1.0)
    gate_proj = gaussian(keys[4], (EXPERTS, D, FE), D ** -0.5, 0.125, ((0, 64), (2, 2)))
    up_proj = gaussian(keys[5], (EXPERTS, D, FE), D ** -0.5, 0.125, ((0, 64), (2, 2)))
    down_proj = gaussian(keys[6], (EXPERTS, FE, D), FE ** -0.5, 0.125, ((0, 64), (1, 2)))
    post_gain = jnp.clip(1.0 + 0.18 * jax.random.normal(keys[7], (D,), jnp.float32), 0.1, 1.9)
    return {"inputs": inputs, "pre_gain": pre_gain, "expert_ids": expert_ids, "route_weights": route_weights, "gate_proj": gate_proj, "up_proj": up_proj, "down_proj": down_proj, "post_gain": post_gain}


EPSILON = 1e-06
LIMIT = 7.0
ALPHA = 1.702

def norm_rows(values, gain):
    floats = values.astype(jnp.float32)
    return floats * lax.rsqrt(lax.optimization_barrier(jnp.mean(floats * floats, axis=-1, keepdims=True)) + EPSILON) * gain

def activate(gate, up):
    gate = jnp.minimum(gate, LIMIT)
    up = jnp.clip(up, -LIMIT, LIMIT)
    return ((up + 1.0) * gate * jax.nn.sigmoid(ALPHA * gate)).astype(jnp.bfloat16)

def reference(inputs, pre_gain, expert_ids, route_weights, gate_proj, up_proj, down_proj, post_gain):
    devices_all = N_EP * N_TP
    normed = norm_rows(inputs, pre_gain).astype(jnp.bfloat16)
    blocks = expert_ids.reshape(devices_all, TOK_DEV * TOP_K)
    one_hot = (blocks[:, :, None] == jnp.arange(EXPERTS, dtype=jnp.int32)[None, None, :]).astype(jnp.int32)
    earlier = jnp.cumsum(one_hot, axis=1) - one_hot
    slot = lax.optimization_barrier(jnp.sum(earlier * one_hot, axis=-1))
    source = jnp.arange(devices_all, dtype=jnp.int32)[:, None]
    target = (blocks * (devices_all * CAP) + source * CAP + slot).reshape(-1).astype(jnp.int32)
    copies = jnp.repeat(normed, TOP_K, axis=0)
    buffer = jnp.zeros((EXPERTS * devices_all * CAP, D), jnp.bfloat16).at[target].set(copies)
    buffer = buffer.reshape(EXPERTS, devices_all * CAP, D)
    half = FE // N_TP

    def one_expert(operands):
        rows, w_gate, w_up, w_down = operands
        gate = jnp.dot(rows, w_gate, preferred_element_type=jnp.float32)
        up = jnp.dot(rows, w_up, preferred_element_type=jnp.float32)
        hidden = activate(gate, up)
        total = jnp.zeros((rows.shape[0], D), jnp.float32)
        for index in range(N_TP):
            part = jnp.dot(hidden[:, index * half:(index + 1) * half], w_down[index * half:(index + 1) * half], preferred_element_type=jnp.float32)
            part = lax.optimization_barrier(part.astype(jnp.bfloat16))
            total = total + part.astype(jnp.float32)
        return total.astype(jnp.bfloat16)
    results = lax.map(one_expert, (buffer, gate_proj, up_proj, down_proj)).reshape(-1, D)
    picked = results[target].reshape(TOKENS, TOP_K, D).astype(jnp.float32)
    mixed = lax.optimization_barrier(jnp.sum(picked * route_weights[:, :, None], axis=1))
    return norm_rows(mixed, post_gain).astype(jnp.bfloat16)
```

```python
import functools

import jax
import jax.numpy as jnp
from jax import lax
from jax.experimental import pallas as pl
from jax.experimental.pallas import tpu as pltpu
from jax.sharding import PartitionSpec as P

EPSILON = 1e-06
LIMIT = 7.0
ALPHA = 1.702
MESH = pl.DeviceIdType.MESH

N_EP = 64
CAP = 12
SLAB = 4
SLABS = CAP // SLAB
TILE = 256


def norm_rows(floats, gain):
    return floats * lax.rsqrt(jnp.mean(floats * floats, axis=-1, keepdims=True) + EPSILON) * gain


def offset_device(ep, o, sign):
    a, b, c = o % 4, (o // 4) % 4, o // 16
    ox, oy, oz = a, (b + a) % 4, (c + b) % 4
    x, y, z = ep % 4, (ep // 4) % 4, ep // 16
    return (
        ((z + sign * oz + 4) % 4) * 16 + ((y + sign * oy + 4) % 4) * 4 + (x + sign * ox + 4) % 4
    )


def kernel(
    chunks,
    x_ref,
    pre_ref,
    ids_ref,
    route_ref,
    gate_ref,
    up_ref,
    down_ref,
    post_ref,
    out_ref,
    x_buf,
    normed,
    place,
    pick0,
    pick1,
    send,
    recv,
    wg,
    wu,
    wd,
    rows,
    hidden,
    back,
    ret,
    total,
    load_sem,
    w_load,
    w_send,
    w_recv,
    s_send,
    s_recv,
    r_send,
    r_recv,
):
    ep = lax.axis_index("ep")
    tp = lax.axis_index("tp")
    tokens, width = x_buf.shape
    half = wg.shape[2]
    per = N_EP // chunks
    chunk_rows = per * CAP
    chunk_slabs = per * SLABS

    x_copy = pltpu.make_async_copy(x_ref, x_buf, load_sem)
    x_copy.start()
    weights = ((gate_ref, wg), (up_ref, wu), (down_ref, wd))
    for n, (source, target) in enumerate(weights):
        pltpu.make_async_copy(source, target.at[tp], w_load.at[n]).start()

    barrier = pltpu.get_barrier_semaphore()

    def greet(o, carry):
        pl.semaphore_signal(
            barrier, inc=1, device_id=((ep + o) % N_EP, tp), device_id_type=MESH
        )
        return carry

    lax.fori_loop(1, N_EP, greet, 0)
    pl.semaphore_signal(barrier, inc=1, device_id=(ep, 1 - tp), device_id_type=MESH)

    ids = ids_ref[...]
    route = route_ref[...]
    expert = lax.broadcasted_iota(jnp.int32, (N_EP, tokens), 0)
    hot0 = (expert == ids[0:1, :]).astype(jnp.bfloat16)
    hot1 = (expert == ids[1:2, :]).astype(jnp.bfloat16)
    row = lax.broadcasted_iota(jnp.int32, (tokens, tokens), 0)
    column = lax.broadcasted_iota(jnp.int32, (tokens, tokens), 1)
    before = (row < column).astype(jnp.bfloat16)
    count0 = jnp.dot(hot0, before, preferred_element_type=jnp.float32)
    count1 = jnp.dot(hot1, before, preferred_element_type=jnp.float32)
    hot0 = hot0.astype(jnp.float32)
    hot1 = hot1.astype(jnp.float32)
    count1 = count1 + jnp.sum(hot0, axis=1, keepdims=True)
    slot0 = jnp.sum(hot0 * count0, axis=0, keepdims=True)
    slot1 = jnp.sum(hot1 * count1, axis=0, keepdims=True)
    x_me, y_me, z_me = ep % 4, (ep // 4) % 4, ep // 16
    a = (ids % 4 - x_me + 4) % 4
    b = ((ids // 4) % 4 - y_me - a + 8) % 4
    c = (ids // 16 - z_me - b + 8) % 4
    order = (a + 4 * b + 16 * c).astype(jnp.float32) * float(CAP)
    target0 = order[0:1, :] + slot0
    target1 = order[1:2, :] + slot1
    slots = N_EP * CAP
    slot_rows = lax.broadcasted_iota(jnp.int32, (slots, tokens), 0).astype(jnp.float32)
    place[...] = jnp.where(
        (slot_rows == target0) | (slot_rows == target1), 1.0, 0.0
    ).astype(jnp.bfloat16)
    diagonal = row == column

    def upright(line):
        return jnp.sum(jnp.where(diagonal, line, 0.0), axis=1, keepdims=True)

    x_copy.wait()
    pre_gain = pre_ref[...]
    step_rows = 32

    def norm_step(i, carry):
        here = pl.ds(pl.multiple_of(i * step_rows, step_rows), step_rows)
        normed[here, :] = norm_rows(x_buf[here, :].astype(jnp.float32), pre_gain).astype(
            jnp.bfloat16
        )
        return carry

    lax.fori_loop(0, tokens // step_rows, norm_step, 0)

    pl.semaphore_wait(barrier, N_EP)

    def message(buffer, o):
        return buffer.at[pl.ds(o * SLABS, SLABS)]

    def outgoing(o):
        return pltpu.make_async_remote_copy(
            src_ref=message(send, o),
            dst_ref=message(recv, o),
            send_sem=s_send.at[o],
            recv_sem=s_recv.at[o],
            device_id=(offset_device(ep, o, 1), tp),
            device_id_type=MESH,
        )

    def returning(o):
        return pltpu.make_async_remote_copy(
            src_ref=message(back, o),
            dst_ref=message(ret, o),
            send_sem=r_send.at[o],
            recv_sem=r_recv.at[o],
            device_id=(offset_device(ep, o, -1), tp),
            device_id_type=MESH,
        )

    own_out = pltpu.make_async_copy(message(send, 0), message(recv, 0), s_recv.at[0])
    own_back = pltpu.make_async_copy(message(back, 0), message(ret, 0), r_recv.at[0])

    def partner_copy(n):
        source, target = weights[n]
        return pltpu.make_async_remote_copy(
            src_ref=source,
            dst_ref=target.at[tp],
            send_sem=w_send.at[n],
            recv_sem=w_recv.at[n],
            device_id=(ep, 1 - tp),
            device_id_type=MESH,
        )

    def chunk_slice(i):
        return pl.ds(pl.multiple_of(i * chunk_slabs, chunk_slabs), chunk_slabs)

    def dispatch(i, carry):
        which = place[pl.ds(pl.multiple_of(i * chunk_rows, chunk_rows), chunk_rows), :]
        for n in range(width // 512):
            columns = slice(n * 512, (n + 1) * 512)
            sent = jnp.dot(which, normed[:, columns], preferred_element_type=jnp.float32)
            send[chunk_slice(i), :, columns] = sent.astype(jnp.bfloat16).reshape(
                chunk_slabs, SLAB, 512
            )

        @pl.when(i == 0)
        def _():
            own_out.start()

        def go(o, carry):
            outgoing(o).start()
            return carry

        lax.fori_loop(jnp.maximum(i * per, 1), (i + 1) * per, go, 0)

        @pl.when(i == 0)
        def _():
            for n in range(3):
                partner_copy(n).start()

        return carry

    lax.fori_loop(0, chunks, dispatch, 0)

    up0, up1 = upright(target0), upright(target1)
    slot_columns = lax.broadcasted_iota(jnp.int32, (tokens, chunk_rows), 1).astype(jnp.float32)
    for i in range(chunks):
        pick0[i] = jnp.where(slot_columns + float(i * chunk_rows) == up0, 1.0, 0.0).astype(
            jnp.bfloat16
        )
        pick1[i] = jnp.where(slot_columns + float(i * chunk_rows) == up1, 1.0, 0.0).astype(
            jnp.bfloat16
        )
    weight0, weight1 = upright(route[0:1, :]), upright(route[1:2, :])

    for n in range(2):
        pltpu.make_async_copy(weights[n][0], weights[n][1].at[tp], w_load.at[n]).wait()
        partner_copy(n).wait_recv()

    def serve(i, carry):
        def arrive(o, carry):
            outgoing(o).wait_recv()
            return carry

        @pl.when(i == 0)
        def _():
            own_out.wait()

        lax.fori_loop(jnp.maximum(i * per, 1), (i + 1) * per, arrive, 0)
        rows[...] = recv[chunk_slice(i)].reshape(chunk_rows, width)

        for h in range(2):

            def expand(n, carry):
                columns = pl.ds(pl.multiple_of(n * TILE, TILE), TILE)
                gate = jnp.dot(rows[...], wg[h, :, columns], preferred_element_type=jnp.float32)
                up = jnp.dot(rows[...], wu[h, :, columns], preferred_element_type=jnp.float32)
                gate = jnp.minimum(gate, LIMIT)
                up = jnp.clip(up, -LIMIT, LIMIT)
                hidden[h, :, columns] = (
                    (up + 1.0) * gate * jax.nn.sigmoid(ALPHA * gate)
                ).astype(jnp.bfloat16)
                return carry

            lax.fori_loop(0, half // TILE, expand, 0)

        @pl.when(i == 0)
        def _():
            pltpu.make_async_copy(weights[2][0], weights[2][1].at[tp], w_load.at[2]).wait()
            partner_copy(2).wait_recv()

        def contract(n, carry):
            columns = pl.ds(pl.multiple_of(n * TILE, TILE), TILE)
            part0 = jnp.dot(hidden[0], wd[0, :, columns], preferred_element_type=jnp.float32)
            part1 = jnp.dot(hidden[1], wd[1, :, columns], preferred_element_type=jnp.float32)
            both = part0.astype(jnp.bfloat16).astype(jnp.float32) + part1.astype(
                jnp.bfloat16
            ).astype(jnp.float32)
            back[chunk_slice(i), :, columns] = both.astype(jnp.bfloat16).reshape(
                chunk_slabs, SLAB, TILE
            )
            return carry

        lax.fori_loop(0, width // TILE, contract, 0)

        @pl.when(i == 0)
        def _():
            own_back.start()

        def go(o, carry):
            returning(o).start()
            return carry

        lax.fori_loop(jnp.maximum(i * per, 1), (i + 1) * per, go, 0)
        return carry

    lax.fori_loop(0, chunks, serve, 0)

    def collect(i, carry):
        def arrive(o, carry):
            returning(o).wait_recv()
            return carry

        @pl.when(i == 0)
        def _():
            own_back.wait()

        lax.fori_loop(jnp.maximum(i * per, 1), (i + 1) * per, arrive, 0)
        for n in range(width // 512):
            columns = slice(n * 512, (n + 1) * 512)
            came = ret[chunk_slice(i), :, columns].reshape(chunk_rows, 512)
            mine = (
                jnp.dot(pick0[i], came, preferred_element_type=jnp.float32) * weight0
                + jnp.dot(pick1[i], came, preferred_element_type=jnp.float32) * weight1
            )

            @pl.when(i == 0)
            def _():
                total[:, columns] = mine

            @pl.when(i > 0)
            def _():
                total[:, columns] += mine

        return carry

    lax.fori_loop(0, chunks, collect, 0)

    post_gain = post_ref[...]

    def finish(i, carry):
        here = pl.ds(pl.multiple_of(i * step_rows, step_rows), step_rows)
        out_ref[here, :] = norm_rows(total[here, :], post_gain).astype(jnp.bfloat16)
        return carry

    lax.fori_loop(0, tokens // step_rows, finish, 0)

    def sent(o, carry):
        outgoing(o).wait_send()
        returning(o).wait_send()
        return carry

    lax.fori_loop(1, N_EP, sent, 0)
    for n in range(3):
        partner_copy(n).wait_send()


def local(inputs, pre_gain, expert_ids, route_weights, gate_proj, up_proj, down_proj, post_gain):
    tokens, width = inputs.shape
    half = gate_proj.shape[2]
    chunks = 4
    chunk_rows = N_EP // chunks * CAP
    slabs = N_EP * SLABS
    bf16, f32 = jnp.bfloat16, jnp.float32
    vmem = pl.BlockSpec(memory_space=pltpu.VMEM)
    hbm = pl.BlockSpec(memory_space=pl.ANY)
    dma = pltpu.SemaphoreType.DMA
    return pl.pallas_call(
        functools.partial(kernel, chunks),
        out_shape=jax.ShapeDtypeStruct((tokens, width), bf16),
        in_specs=[hbm, vmem, vmem, vmem, hbm, hbm, hbm, vmem],
        out_specs=vmem,
        scratch_shapes=[
            pltpu.VMEM((tokens, width), bf16),
            pltpu.VMEM((tokens, width), bf16),
            pltpu.VMEM((N_EP * CAP, tokens), bf16),
            pltpu.VMEM((chunks, tokens, chunk_rows), bf16),
            pltpu.VMEM((chunks, tokens, chunk_rows), bf16),
            pltpu.VMEM((slabs, SLAB, width), bf16),
            pltpu.VMEM((slabs, SLAB, width), bf16),
            pltpu.VMEM((2, width, half), bf16),
            pltpu.VMEM((2, width, half), bf16),
            pltpu.VMEM((2, half, width), bf16),
            pltpu.VMEM((chunk_rows, width), bf16),
            pltpu.VMEM((2, chunk_rows, half), bf16),
            pltpu.VMEM((slabs, SLAB, width), bf16),
            pltpu.VMEM((slabs, SLAB, width), bf16),
            pltpu.VMEM((tokens, width), f32),
            dma,
            dma((3,)),
            dma((3,)),
            dma((3,)),
            dma((N_EP,)),
            dma((N_EP,)),
            dma((N_EP,)),
            dma((N_EP,)),
        ],
        compiler_params=pltpu.CompilerParams(
            collective_id=0, has_side_effects=True, vmem_limit_bytes=60 * 1024 * 1024
        ),
    )(
        inputs,
        pre_gain.reshape(1, width),
        expert_ids.T,
        route_weights.T,
        gate_proj[0],
        up_proj[0],
        down_proj[0],
        post_gain.reshape(1, width),
    )


def solution(mesh):
    in_specs = (
        P(("ep", "tp"), None),
        P(),
        P(("ep", "tp"), None),
        P(("ep", "tp"), None),
        P("ep", None, "tp"),
        P("ep", None, "tp"),
        P("ep", "tp", None),
        P(),
    )
    out_specs = P(("ep", "tp"), None)
    return jax.shard_map(local, mesh=mesh, in_specs=in_specs, out_specs=out_specs, check_vma=False)
```

```python
import functools

import jax
import jax.numpy as jnp
from jax import lax
from jax.experimental import pallas as pl
from jax.experimental.pallas import tpu as pltpu
from jax.sharding import PartitionSpec as P

EPSILON = 1e-06
LIMIT = 7.0
ALPHA = 1.702
MESH = pl.DeviceIdType.MESH

N_EP = 64
CAP = 12
SLAB = 4
SLABS = CAP // SLAB
TILE = 256


def norm_rows(floats, gain):
    return floats * lax.rsqrt(jnp.mean(floats * floats, axis=-1, keepdims=True) + EPSILON) * gain


def offset_device(ep, o, sign):
    a, b, c = o % 4, (o // 4) % 4, o // 16
    ox, oy, oz = a, (a + b) % 4, (a + b + c) % 4
    x, y, z = ep % 4, (ep // 4) % 4, ep // 16
    return (
        ((z + sign * oz + 4) % 4) * 16 + ((y + sign * oy + 4) % 4) * 4 + (x + sign * ox + 4) % 4
    )


def kernel(
    chunks,
    x_ref,
    pre_ref,
    ids_ref,
    route_ref,
    gate_ref,
    up_ref,
    down_ref,
    post_ref,
    out_ref,
    x_buf,
    normed,
    place,
    pick0,
    pick1,
    send,
    recv,
    wg,
    wu,
    wd,
    rows,
    hidden,
    back,
    ret,
    total,
    load_sem,
    w_load,
    w_send,
    w_recv,
    s_send,
    s_recv,
    r_send,
    r_recv,
):
    ep = lax.axis_index("ep")
    tp = lax.axis_index("tp")
    tokens, width = x_buf.shape
    half = wg.shape[2]
    per = N_EP // chunks
    chunk_rows = per * CAP
    chunk_slabs = per * SLABS

    x_copy = pltpu.make_async_copy(x_ref, x_buf, load_sem)
    x_copy.start()
    weights = ((gate_ref, wg), (up_ref, wu), (down_ref, wd))
    for n, (source, target) in enumerate(weights):
        pltpu.make_async_copy(source, target.at[tp], w_load.at[n]).start()

    barrier = pltpu.get_barrier_semaphore()

    def greet(o, carry):
        pl.semaphore_signal(
            barrier, inc=1, device_id=((ep + o) % N_EP, tp), device_id_type=MESH
        )
        return carry

    lax.fori_loop(1, N_EP, greet, 0)
    pl.semaphore_signal(barrier, inc=1, device_id=(ep, 1 - tp), device_id_type=MESH)

    ids = ids_ref[...]
    route = route_ref[...]
    expert = lax.broadcasted_iota(jnp.int32, (N_EP, tokens), 0)
    hot0 = (expert == ids[0:1, :]).astype(jnp.bfloat16)
    hot1 = (expert == ids[1:2, :]).astype(jnp.bfloat16)
    row = lax.broadcasted_iota(jnp.int32, (tokens, tokens), 0)
    column = lax.broadcasted_iota(jnp.int32, (tokens, tokens), 1)
    before = (row < column).astype(jnp.bfloat16)
    count0 = jnp.dot(hot0, before, preferred_element_type=jnp.float32)
    count1 = jnp.dot(hot1, before, preferred_element_type=jnp.float32)
    hot0 = hot0.astype(jnp.float32)
    hot1 = hot1.astype(jnp.float32)
    count1 = count1 + jnp.sum(hot0, axis=1, keepdims=True)
    slot0 = jnp.sum(hot0 * count0, axis=0, keepdims=True)
    slot1 = jnp.sum(hot1 * count1, axis=0, keepdims=True)
    x_me, y_me, z_me = ep % 4, (ep // 4) % 4, ep // 16
    a = (ids % 4 - x_me + 4) % 4
    b = ((ids // 4) % 4 - y_me - a + 8) % 4
    c = (ids // 16 - z_me - a - b + 12) % 4
    order = (a + 4 * b + 16 * c).astype(jnp.float32) * float(CAP)
    target0 = order[0:1, :] + slot0
    target1 = order[1:2, :] + slot1
    slots = N_EP * CAP
    slot_rows = lax.broadcasted_iota(jnp.int32, (slots, tokens), 0).astype(jnp.float32)
    place[...] = jnp.where(
        (slot_rows == target0) | (slot_rows == target1), 1.0, 0.0
    ).astype(jnp.bfloat16)
    diagonal = row == column

    def upright(line):
        return jnp.sum(jnp.where(diagonal, line, 0.0), axis=1, keepdims=True)

    x_copy.wait()
    pre_gain = pre_ref[...]
    step_rows = 32

    def norm_step(i, carry):
        here = pl.ds(pl.multiple_of(i * step_rows, step_rows), step_rows)
        normed[here, :] = norm_rows(x_buf[here, :].astype(jnp.float32), pre_gain).astype(
            jnp.bfloat16
        )
        return carry

    lax.fori_loop(0, tokens // step_rows, norm_step, 0)


    def message(buffer, o):
        return buffer.at[pl.ds(o * SLABS, SLABS)]

    def outgoing(o):
        return pltpu.make_async_remote_copy(
            src_ref=message(send, o),
            dst_ref=message(recv, o),
            send_sem=s_send.at[o],
            recv_sem=s_recv.at[o],
            device_id=(offset_device(ep, o, 1), tp),
            device_id_type=MESH,
        )

    def returning(o):
        return pltpu.make_async_remote_copy(
            src_ref=message(back, o),
            dst_ref=message(ret, o),
            send_sem=r_send.at[o],
            recv_sem=r_recv.at[o],
            device_id=(offset_device(ep, o, -1), tp),
            device_id_type=MESH,
        )

    own_out = pltpu.make_async_copy(message(send, 0), message(recv, 0), s_recv.at[0])
    own_back = pltpu.make_async_copy(message(back, 0), message(ret, 0), r_recv.at[0])

    def partner_copy(n):
        source, target = weights[n]
        return pltpu.make_async_remote_copy(
            src_ref=source,
            dst_ref=target.at[tp],
            send_sem=w_send.at[n],
            recv_sem=w_recv.at[n],
            device_id=(ep, 1 - tp),
            device_id_type=MESH,
        )

    def chunk_slice(i):
        return pl.ds(pl.multiple_of(i * chunk_slabs, chunk_slabs), chunk_slabs)

    def dispatch(i, carry):
        which = place[pl.ds(pl.multiple_of(i * chunk_rows, chunk_rows), chunk_rows), :]
        for n in range(width // 512):
            columns = slice(n * 512, (n + 1) * 512)
            sent = jnp.dot(which, normed[:, columns], preferred_element_type=jnp.float32)
            send[chunk_slice(i), :, columns] = sent.astype(jnp.bfloat16).reshape(
                chunk_slabs, SLAB, 512
            )

        @pl.when(i == 0)
        def _():
            pl.semaphore_wait(barrier, N_EP)
            own_out.start()

        def go(o, carry):
            outgoing(o).start()
            return carry

        lax.fori_loop(jnp.maximum(i * per, 1), (i + 1) * per, go, 0)

        @pl.when(i == 0)
        def _():
            for n in range(3):
                partner_copy(n).start()

        return carry

    lax.fori_loop(0, chunks, dispatch, 0)

    up0, up1 = upright(target0), upright(target1)
    slot_columns = lax.broadcasted_iota(jnp.int32, (tokens, chunk_rows), 1).astype(jnp.float32)
    for i in range(chunks):
        pick0[i] = jnp.where(slot_columns + float(i * chunk_rows) == up0, 1.0, 0.0).astype(
            jnp.bfloat16
        )
        pick1[i] = jnp.where(slot_columns + float(i * chunk_rows) == up1, 1.0, 0.0).astype(
            jnp.bfloat16
        )
    weight0, weight1 = upright(route[0:1, :]), upright(route[1:2, :])

    for n in range(2):
        pltpu.make_async_copy(weights[n][0], weights[n][1].at[tp], w_load.at[n]).wait()
        partner_copy(n).wait_recv()

    def serve(i, carry):
        def arrive(o, carry):
            outgoing(o).wait_recv()
            return carry

        @pl.when(i == 0)
        def _():
            own_out.wait()

        lax.fori_loop(jnp.maximum(i * per, 1), (i + 1) * per, arrive, 0)
        rows[...] = recv[chunk_slice(i)].reshape(chunk_rows, width)

        for h in range(2):

            def expand(n, carry):
                columns = pl.ds(pl.multiple_of(n * TILE, TILE), TILE)
                gate = jnp.dot(rows[...], wg[h, :, columns], preferred_element_type=jnp.float32)
                up = jnp.dot(rows[...], wu[h, :, columns], preferred_element_type=jnp.float32)
                gate = jnp.minimum(gate, LIMIT)
                up = jnp.clip(up, -LIMIT, LIMIT)
                hidden[h, :, columns] = (
                    (up + 1.0) * gate * jax.nn.sigmoid(ALPHA * gate)
                ).astype(jnp.bfloat16)
                return carry

            lax.fori_loop(0, half // TILE, expand, 0)

        @pl.when(i == 0)
        def _():
            pltpu.make_async_copy(weights[2][0], weights[2][1].at[tp], w_load.at[2]).wait()
            partner_copy(2).wait_recv()

        def contract(n, carry):
            columns = pl.ds(pl.multiple_of(n * 512, 512), 512)
            part0 = jnp.dot(hidden[0], wd[0, :, columns], preferred_element_type=jnp.float32)
            part1 = jnp.dot(hidden[1], wd[1, :, columns], preferred_element_type=jnp.float32)
            both = part0.astype(jnp.bfloat16).astype(jnp.float32) + part1.astype(
                jnp.bfloat16
            ).astype(jnp.float32)
            back[chunk_slice(i), :, columns] = both.astype(jnp.bfloat16).reshape(
                chunk_slabs, SLAB, 512
            )
            return carry

        lax.fori_loop(0, width // 512, contract, 0)

        @pl.when(i == 0)
        def _():
            own_back.start()

        def go(o, carry):
            returning(o).start()
            return carry

        lax.fori_loop(jnp.maximum(i * per, 1), (i + 1) * per, go, 0)
        return carry

    lax.fori_loop(0, chunks, serve, 0)

    def collect(i, carry):
        def arrive(o, carry):
            returning(o).wait_recv()
            return carry

        @pl.when(i == 0)
        def _():
            own_back.wait()

        lax.fori_loop(jnp.maximum(i * per, 1), (i + 1) * per, arrive, 0)
        for n in range(width // 512):
            columns = slice(n * 512, (n + 1) * 512)
            came = ret[chunk_slice(i), :, columns].reshape(chunk_rows, 512)
            mine = (
                jnp.dot(pick0[i], came, preferred_element_type=jnp.float32) * weight0
                + jnp.dot(pick1[i], came, preferred_element_type=jnp.float32) * weight1
            )

            @pl.when(i == 0)
            def _():
                total[:, columns] = mine

            @pl.when(i > 0)
            def _():
                total[:, columns] += mine

        return carry

    lax.fori_loop(0, chunks, collect, 0)

    post_gain = post_ref[...]

    def finish(i, carry):
        here = pl.ds(pl.multiple_of(i * step_rows, step_rows), step_rows)
        out_ref[here, :] = norm_rows(total[here, :], post_gain).astype(jnp.bfloat16)
        return carry

    lax.fori_loop(0, tokens // step_rows, finish, 0)

    def sent(o, carry):
        outgoing(o).wait_send()
        returning(o).wait_send()
        return carry

    lax.fori_loop(1, N_EP, sent, 0)
    for n in range(3):
        partner_copy(n).wait_send()


def local(inputs, pre_gain, expert_ids, route_weights, gate_proj, up_proj, down_proj, post_gain):
    tokens, width = inputs.shape
    half = gate_proj.shape[2]
    chunks = 4
    chunk_rows = N_EP // chunks * CAP
    slabs = N_EP * SLABS
    bf16, f32 = jnp.bfloat16, jnp.float32
    vmem = pl.BlockSpec(memory_space=pltpu.VMEM)
    hbm = pl.BlockSpec(memory_space=pl.ANY)
    dma = pltpu.SemaphoreType.DMA
    return pl.pallas_call(
        functools.partial(kernel, chunks),
        out_shape=pltpu.VMEM((tokens, width), bf16),
        in_specs=[hbm, vmem, vmem, vmem, hbm, hbm, hbm, vmem],
        out_specs=vmem,
        scratch_shapes=[
            pltpu.VMEM((tokens, width), bf16),
            pltpu.VMEM((tokens, width), bf16),
            pltpu.VMEM((N_EP * CAP, tokens), bf16),
            pltpu.VMEM((chunks, tokens, chunk_rows), bf16),
            pltpu.VMEM((chunks, tokens, chunk_rows), bf16),
            pltpu.VMEM((slabs, SLAB, width), bf16),
            pltpu.VMEM((slabs, SLAB, width), bf16),
            pltpu.VMEM((2, width, half), bf16),
            pltpu.VMEM((2, width, half), bf16),
            pltpu.VMEM((2, half, width), bf16),
            pltpu.VMEM((chunk_rows, width), bf16),
            pltpu.VMEM((2, chunk_rows, half), bf16),
            pltpu.VMEM((slabs, SLAB, width), bf16),
            pltpu.VMEM((slabs, SLAB, width), bf16),
            pltpu.VMEM((tokens, width), f32),
            dma,
            dma((3,)),
            dma((3,)),
            dma((3,)),
            dma((N_EP,)),
            dma((N_EP,)),
            dma((N_EP,)),
            dma((N_EP,)),
        ],
        compiler_params=pltpu.CompilerParams(
            collective_id=0, has_side_effects=True, vmem_limit_bytes=60 * 1024 * 1024
        ),
    )(
        inputs,
        pre_gain.reshape(1, width),
        expert_ids.T,
        route_weights.T,
        gate_proj[0],
        up_proj[0],
        down_proj[0],
        post_gain.reshape(1, width),
    )


def solution(mesh):
    in_specs = (
        P(("ep", "tp"), None),
        P(),
        P(("ep", "tp"), None),
        P(("ep", "tp"), None),
        P("ep", None, "tp"),
        P("ep", None, "tp"),
        P("ep", "tp", None),
        P(),
    )
    out_specs = P(("ep", "tp"), None)
    return jax.shard_map(local, mesh=mesh, in_specs=in_specs, out_specs=out_specs, check_vma=False)
```

```python
import functools

import jax
import jax.numpy as jnp
from jax import lax
from jax.experimental import pallas as pl
from jax.experimental.pallas import tpu as pltpu
from jax.sharding import PartitionSpec as P

EPSILON = 1e-06
LIMIT = 7.0
ALPHA = 1.702
MESH = pl.DeviceIdType.MESH

N_EP = 64
CAP = 12
SLAB = 4
SLABS = CAP // SLAB
TILE = 256
PARTS = 2


def norm_rows(floats, gain):
    return floats * lax.rsqrt(jnp.mean(floats * floats, axis=-1, keepdims=True) + EPSILON) * gain


def offset_device(ep, o, sign):
    a, b, c = o % 4, (o // 4) % 4, o // 16
    ox, oy, oz = a, (a + b) % 4, (a + b + c) % 4
    x, y, z = ep % 4, (ep // 4) % 4, ep // 16
    return (
        ((z + sign * oz + 4) % 4) * 16 + ((y + sign * oy + 4) % 4) * 4 + (x + sign * ox + 4) % 4
    )


def kernel(
    chunks,
    x_ref,
    pre_ref,
    ids_ref,
    route_ref,
    gate_ref,
    up_ref,
    down_ref,
    post_ref,
    out_ref,
    x_buf,
    normed,
    place,
    pick0,
    pick1,
    send,
    recv,
    wg,
    wu,
    wd,
    rows,
    hidden,
    back,
    ret,
    total,
    load_sem,
    w_load,
    w_send,
    w_recv,
    s_send,
    s_recv,
    r_send,
    r_recv,
):
    ep = lax.axis_index("ep")
    tp = lax.axis_index("tp")
    tokens, width = x_buf.shape
    half = wg.shape[2]
    per = N_EP // chunks
    chunk_rows = per * CAP
    chunk_slabs = per * SLABS

    x_copy = pltpu.make_async_copy(x_ref, x_buf, load_sem)
    x_copy.start()
    weights = ((gate_ref, wg), (up_ref, wu), (down_ref, wd))
    for n, (source, target) in enumerate(weights):
        pltpu.make_async_copy(source, target.at[tp], w_load.at[n]).start()

    barrier = pltpu.get_barrier_semaphore()

    def greet(o, carry):
        pl.semaphore_signal(
            barrier, inc=1, device_id=((ep + o) % N_EP, tp), device_id_type=MESH
        )
        return carry

    lax.fori_loop(1, N_EP, greet, 0)
    pl.semaphore_signal(barrier, inc=1, device_id=(ep, 1 - tp), device_id_type=MESH)

    ids = ids_ref[...]
    route = route_ref[...]
    expert = lax.broadcasted_iota(jnp.int32, (N_EP, tokens), 0)
    hot0 = (expert == ids[0:1, :]).astype(jnp.bfloat16)
    hot1 = (expert == ids[1:2, :]).astype(jnp.bfloat16)
    row = lax.broadcasted_iota(jnp.int32, (tokens, tokens), 0)
    column = lax.broadcasted_iota(jnp.int32, (tokens, tokens), 1)
    before = (row < column).astype(jnp.bfloat16)
    count0 = jnp.dot(hot0, before, preferred_element_type=jnp.float32)
    count1 = jnp.dot(hot1, before, preferred_element_type=jnp.float32)
    hot0 = hot0.astype(jnp.float32)
    hot1 = hot1.astype(jnp.float32)
    count1 = count1 + jnp.sum(hot0, axis=1, keepdims=True)
    slot0 = jnp.sum(hot0 * count0, axis=0, keepdims=True)
    slot1 = jnp.sum(hot1 * count1, axis=0, keepdims=True)
    x_me, y_me, z_me = ep % 4, (ep // 4) % 4, ep // 16
    a = (ids % 4 - x_me + 4) % 4
    b = ((ids // 4) % 4 - y_me - a + 8) % 4
    c = (ids // 16 - z_me - a - b + 12) % 4
    order = (a + 4 * b + 16 * c).astype(jnp.float32) * float(CAP)
    target0 = order[0:1, :] + slot0
    target1 = order[1:2, :] + slot1
    slots = N_EP * CAP
    slot_rows = lax.broadcasted_iota(jnp.int32, (slots, tokens), 0).astype(jnp.float32)
    place[...] = jnp.where(
        (slot_rows == target0) | (slot_rows == target1), 1.0, 0.0
    ).astype(jnp.bfloat16)
    diagonal = row == column

    def upright(line):
        return jnp.sum(jnp.where(diagonal, line, 0.0), axis=1, keepdims=True)

    x_copy.wait()
    pre_gain = pre_ref[...]
    step_rows = 32

    def norm_step(i, carry):
        here = pl.ds(pl.multiple_of(i * step_rows, step_rows), step_rows)
        normed[here, :] = norm_rows(x_buf[here, :].astype(jnp.float32), pre_gain).astype(
            jnp.bfloat16
        )
        return carry

    lax.fori_loop(0, tokens // step_rows, norm_step, 0)


    def message(buffer, o):
        return buffer.at[pl.ds(o * SLABS, SLABS)]

    def outgoing(o):
        return pltpu.make_async_remote_copy(
            src_ref=message(send, o),
            dst_ref=message(recv, o),
            send_sem=s_send.at[o],
            recv_sem=s_recv.at[o],
            device_id=(offset_device(ep, o, 1), tp),
            device_id_type=MESH,
        )

    def returning(o):
        return pltpu.make_async_remote_copy(
            src_ref=message(back, o),
            dst_ref=message(ret, o),
            send_sem=r_send.at[o],
            recv_sem=r_recv.at[o],
            device_id=(offset_device(ep, o, -1), tp),
            device_id_type=MESH,
        )

    def returning_part(o, n):
        columns = pl.ds(n * (width // PARTS), width // PARTS)
        return pltpu.make_async_remote_copy(
            src_ref=back.at[pl.ds(o * SLABS, SLABS), :, columns],
            dst_ref=ret.at[pl.ds(o * SLABS, SLABS), :, columns],
            send_sem=r_send.at[o + n * per],
            recv_sem=r_recv.at[o + n * per],
            device_id=(offset_device(ep, o, -1), tp),
            device_id_type=MESH,
        )

    own_out = pltpu.make_async_copy(message(send, 0), message(recv, 0), s_recv.at[0])
    own_back = pltpu.make_async_copy(message(back, 0), message(ret, 0), r_recv.at[0])

    def partner_copy(n):
        source, target = weights[n]
        return pltpu.make_async_remote_copy(
            src_ref=source,
            dst_ref=target.at[tp],
            send_sem=w_send.at[n],
            recv_sem=w_recv.at[n],
            device_id=(ep, 1 - tp),
            device_id_type=MESH,
        )

    def chunk_slice(i):
        return pl.ds(pl.multiple_of(i * chunk_slabs, chunk_slabs), chunk_slabs)

    def dispatch(i, carry):
        which = place[pl.ds(pl.multiple_of(i * chunk_rows, chunk_rows), chunk_rows), :]
        for n in range(width // 512):
            columns = slice(n * 512, (n + 1) * 512)
            sent = jnp.dot(which, normed[:, columns], preferred_element_type=jnp.float32)
            send[chunk_slice(i), :, columns] = sent.astype(jnp.bfloat16).reshape(
                chunk_slabs, SLAB, 512
            )

        @pl.when(i == 0)
        def _():
            pl.semaphore_wait(barrier, N_EP)
            own_out.start()

        def go(o, carry):
            outgoing(o).start()
            return carry

        lax.fori_loop(jnp.maximum(i * per, 1), (i + 1) * per, go, 0)

        @pl.when(i == 0)
        def _():
            for n in range(3):
                partner_copy(n).start()

        return carry

    lax.fori_loop(0, chunks, dispatch, 0)

    up0, up1 = upright(target0), upright(target1)
    slot_columns = lax.broadcasted_iota(jnp.int32, (tokens, chunk_rows), 1).astype(jnp.float32)
    for i in range(chunks):
        pick0[i] = jnp.where(slot_columns + float(i * chunk_rows) == up0, 1.0, 0.0).astype(
            jnp.bfloat16
        )
        pick1[i] = jnp.where(slot_columns + float(i * chunk_rows) == up1, 1.0, 0.0).astype(
            jnp.bfloat16
        )
    weight0, weight1 = upright(route[0:1, :]), upright(route[1:2, :])

    for n in range(2):
        pltpu.make_async_copy(weights[n][0], weights[n][1].at[tp], w_load.at[n]).wait()
        partner_copy(n).wait_recv()

    def serve(i, carry):
        def arrive(o, carry):
            outgoing(o).wait_recv()
            return carry

        @pl.when(i == 0)
        def _():
            own_out.wait()

        lax.fori_loop(jnp.maximum(i * per, 1), (i + 1) * per, arrive, 0)
        rows[...] = recv[chunk_slice(i)].reshape(chunk_rows, width)

        for h in range(2):

            def expand(n, carry):
                columns = pl.ds(pl.multiple_of(n * TILE, TILE), TILE)
                gate = jnp.dot(rows[...], wg[h, :, columns], preferred_element_type=jnp.float32)
                up = jnp.dot(rows[...], wu[h, :, columns], preferred_element_type=jnp.float32)
                gate = jnp.minimum(gate, LIMIT)
                up = jnp.clip(up, -LIMIT, LIMIT)
                hidden[h, :, columns] = (
                    (up + 1.0) * gate * jax.nn.sigmoid(ALPHA * gate)
                ).astype(jnp.bfloat16)
                return carry

            lax.fori_loop(0, half // TILE, expand, 0)

        @pl.when(i == 0)
        def _():
            pltpu.make_async_copy(weights[2][0], weights[2][1].at[tp], w_load.at[2]).wait()
            partner_copy(2).wait_recv()

        def contract(n, carry):
            columns = pl.ds(pl.multiple_of(n * 512, 512), 512)
            part0 = jnp.dot(hidden[0], wd[0, :, columns], preferred_element_type=jnp.float32)
            part1 = jnp.dot(hidden[1], wd[1, :, columns], preferred_element_type=jnp.float32)
            both = part0.astype(jnp.bfloat16).astype(jnp.float32) + part1.astype(
                jnp.bfloat16
            ).astype(jnp.float32)
            back[chunk_slice(i), :, columns] = both.astype(jnp.bfloat16).reshape(
                chunk_slabs, SLAB, 512
            )
            return carry

        lax.fori_loop(0, width // 512, contract, 0)

        @pl.when(i == 0)
        def _():
            own_back.start()

        def go(o, carry):
            returning(o).start()
            return carry

        @pl.when(i < chunks - 1)
        def _():
            lax.fori_loop(jnp.maximum(i * per, 1), (i + 1) * per, go, 0)

        @pl.when(i == chunks - 1)
        def _():
            for n in range(PARTS):

                def go_part(o, carry):
                    returning_part(o, n).start()
                    return carry

                lax.fori_loop(N_EP - per, N_EP, go_part, 0)

        return carry

    lax.fori_loop(0, chunks, serve, 0)

    def sent(o, carry):
        outgoing(o).wait_send()
        return carry

    lax.fori_loop(1, N_EP, sent, 0)
    for n in range(3):
        partner_copy(n).wait_send()

    def mixed(i, n):
        came = ret[chunk_slice(i), :, n * 512 : (n + 1) * 512].reshape(chunk_rows, 512)
        return (
            jnp.dot(pick0[i], came, preferred_element_type=jnp.float32) * weight0
            + jnp.dot(pick1[i], came, preferred_element_type=jnp.float32) * weight1
        )

    def collect(i, carry):
        def arrive(o, carry):
            returning(o).wait_send()
            returning(o).wait_recv()
            return carry

        @pl.when(i == 0)
        def _():
            own_back.wait()

        lax.fori_loop(jnp.maximum(i * per, 1), (i + 1) * per, arrive, 0)
        for n in range(width // 512):
            mine = mixed(i, n)
            columns = slice(n * 512, (n + 1) * 512)

            @pl.when(i == 0)
            def _():
                total[:, columns] = mine

            @pl.when(i > 0)
            def _():
                total[:, columns] += mine

        return carry

    lax.fori_loop(0, chunks - 1, collect, 0)

    post_gain = post_ref[...]
    squares = jnp.zeros((tokens, 1), jnp.float32)
    last = chunks - 1
    for h in range(PARTS):

        def arrive_part(o, carry):
            returning_part(o, h).wait_send()
            returning_part(o, h).wait_recv()
            return carry

        lax.fori_loop(last * per, N_EP, arrive_part, 0)
        for n in range(h * width // 512 // PARTS, (h + 1) * width // 512 // PARTS):
            columns = slice(n * 512, (n + 1) * 512)
            part = total[:, columns] + mixed(last, n)
            total[:, columns] = part
            squares += jnp.sum(part * part, axis=1, keepdims=True)
    scale = lax.rsqrt(squares / float(width) + EPSILON)
    for n in range(width // 512):
        columns = slice(n * 512, (n + 1) * 512)
        out_ref[:, columns] = (total[:, columns] * scale * post_gain[:, columns]).astype(jnp.bfloat16)


def local(inputs, pre_gain, expert_ids, route_weights, gate_proj, up_proj, down_proj, post_gain):
    tokens, width = inputs.shape
    half = gate_proj.shape[2]
    chunks = 4
    chunk_rows = N_EP // chunks * CAP
    slabs = N_EP * SLABS
    bf16, f32 = jnp.bfloat16, jnp.float32
    vmem = pl.BlockSpec(memory_space=pltpu.VMEM)
    hbm = pl.BlockSpec(memory_space=pl.ANY)
    dma = pltpu.SemaphoreType.DMA
    return pl.pallas_call(
        functools.partial(kernel, chunks),
        out_shape=pltpu.VMEM((tokens, width), bf16),
        in_specs=[hbm, vmem, vmem, vmem, hbm, hbm, hbm, vmem],
        out_specs=vmem,
        scratch_shapes=[
            pltpu.VMEM((tokens, width), bf16),
            pltpu.VMEM((tokens, width), bf16),
            pltpu.VMEM((N_EP * CAP, tokens), bf16),
            pltpu.VMEM((chunks, tokens, chunk_rows), bf16),
            pltpu.VMEM((chunks, tokens, chunk_rows), bf16),
            pltpu.VMEM((slabs, SLAB, width), bf16),
            pltpu.VMEM((slabs, SLAB, width), bf16),
            pltpu.VMEM((2, width, half), bf16),
            pltpu.VMEM((2, width, half), bf16),
            pltpu.VMEM((2, half, width), bf16),
            pltpu.VMEM((chunk_rows, width), bf16),
            pltpu.VMEM((2, chunk_rows, half), bf16),
            pltpu.VMEM((slabs, SLAB, width), bf16),
            pltpu.VMEM((slabs, SLAB, width), bf16),
            pltpu.VMEM((tokens, width), f32),
            dma,
            dma((3,)),
            dma((3,)),
            dma((3,)),
            dma((N_EP,)),
            dma((N_EP,)),
            dma((N_EP + (PARTS - 1) * N_EP // chunks,)),
            dma((N_EP + (PARTS - 1) * N_EP // chunks,)),
        ],
        compiler_params=pltpu.CompilerParams(
            collective_id=0, has_side_effects=True, vmem_limit_bytes=60 * 1024 * 1024
        ),
    )(
        inputs,
        pre_gain.reshape(1, width),
        expert_ids.T,
        route_weights.T,
        gate_proj[0],
        up_proj[0],
        down_proj[0],
        post_gain.reshape(1, width),
    )


def solution(mesh):
    in_specs = (
        P(("ep", "tp"), None),
        P(),
        P(("ep", "tp"), None),
        P(("ep", "tp"), None),
        P("ep", None, "tp"),
        P("ep", None, "tp"),
        P("ep", "tp", None),
        P(),
    )
    out_specs = P(("ep", "tp"), None)
    return jax.shard_map(local, mesh=mesh, in_specs=in_specs, out_specs=out_specs, check_vma=False)
```

```python
import functools

import jax
import jax.numpy as jnp
from jax import lax
from jax.experimental import pallas as pl
from jax.experimental.pallas import tpu as pltpu
from jax.sharding import PartitionSpec as P

EPSILON = 1e-06
LIMIT = 7.0
ALPHA = 1.702
MESH = pl.DeviceIdType.MESH

N_EP = 64
CAP = 12
SLAB = 4
SLABS = CAP // SLAB
TILE = 256
PARTS = 2


def norm_rows(floats, gain):
    return floats * lax.rsqrt(jnp.mean(floats * floats, axis=-1, keepdims=True) + EPSILON) * gain


def offset_device(ep, o, sign):
    a, b, c = o % 4, (o // 4) % 4, o // 16
    ox, oy, oz = a, (a + b) % 4, (a + b + c) % 4
    x, y, z = ep % 4, (ep // 4) % 4, ep // 16
    return (
        ((z + sign * oz + 4) % 4) * 16 + ((y + sign * oy + 4) % 4) * 4 + (x + sign * ox + 4) % 4
    )


def kernel(
    chunks,
    x_ref,
    pre_ref,
    ids_ref,
    route_ref,
    gate_ref,
    up_ref,
    down_ref,
    post_ref,
    out_ref,
    x_buf,
    normed,
    place,
    picks,
    send,
    recv,
    wg,
    wu,
    wd,
    rows,
    hidden,
    back,
    ret,
    total,
    load_sem,
    w_load,
    w_send,
    w_recv,
    s_send,
    s_recv,
    r_send,
    r_recv,
):
    ep = lax.axis_index("ep")
    tp = lax.axis_index("tp")
    tokens, width = x_buf.shape
    half = wg.shape[2]
    per = N_EP // chunks
    chunk_rows = per * CAP
    chunk_slabs = per * SLABS

    x_copy = pltpu.make_async_copy(x_ref, x_buf, load_sem)
    x_copy.start()
    weights = ((gate_ref, wg), (up_ref, wu), (down_ref, wd))
    for n, (source, target) in enumerate(weights):
        pltpu.make_async_copy(source, target.at[tp], w_load.at[n]).start()

    barrier = pltpu.get_barrier_semaphore()

    def greet(o, carry):
        pl.semaphore_signal(
            barrier, inc=1, device_id=((ep + o) % N_EP, tp), device_id_type=MESH
        )
        return carry

    lax.fori_loop(1, N_EP, greet, 0)
    pl.semaphore_signal(barrier, inc=1, device_id=(ep, 1 - tp), device_id_type=MESH)

    ids = ids_ref[...]
    route = route_ref[...]
    expert = lax.broadcasted_iota(jnp.int32, (N_EP, tokens), 0)
    hot0 = (expert == ids[0:1, :]).astype(jnp.bfloat16)
    hot1 = (expert == ids[1:2, :]).astype(jnp.bfloat16)
    row = lax.broadcasted_iota(jnp.int32, (tokens, tokens), 0)
    column = lax.broadcasted_iota(jnp.int32, (tokens, tokens), 1)
    before = (row < column).astype(jnp.bfloat16)
    count0 = jnp.dot(hot0, before, preferred_element_type=jnp.float32)
    count1 = jnp.dot(hot1, before, preferred_element_type=jnp.float32)
    hot0 = hot0.astype(jnp.float32)
    hot1 = hot1.astype(jnp.float32)
    count1 = count1 + jnp.sum(hot0, axis=1, keepdims=True)
    slot0 = jnp.sum(hot0 * count0, axis=0, keepdims=True)
    slot1 = jnp.sum(hot1 * count1, axis=0, keepdims=True)
    x_me, y_me, z_me = ep % 4, (ep // 4) % 4, ep // 16
    a = (ids % 4 - x_me + 4) % 4
    b = ((ids // 4) % 4 - y_me - a + 8) % 4
    c = (ids // 16 - z_me - a - b + 12) % 4
    order = (a + 4 * b + 16 * c).astype(jnp.float32) * float(CAP)
    target0 = order[0:1, :] + slot0
    target1 = order[1:2, :] + slot1
    slots = N_EP * CAP
    slot_rows = lax.broadcasted_iota(jnp.int32, (slots, tokens), 0).astype(jnp.float32)
    place[...] = jnp.where(
        (slot_rows == target0) | (slot_rows == target1), 1.0, 0.0
    ).astype(jnp.bfloat16)
    diagonal = row == column

    def upright(line):
        return jnp.sum(jnp.where(diagonal, line, 0.0), axis=1, keepdims=True)

    x_copy.wait()
    pre_gain = pre_ref[...]
    step_rows = 32

    def norm_step(i, carry):
        here = pl.ds(pl.multiple_of(i * step_rows, step_rows), step_rows)
        normed[here, :] = norm_rows(x_buf[here, :].astype(jnp.float32), pre_gain).astype(
            jnp.bfloat16
        )
        return carry

    lax.fori_loop(0, tokens // step_rows, norm_step, 0)


    def message(buffer, o):
        return buffer.at[pl.ds(o * SLABS, SLABS)]

    def outgoing(o):
        return pltpu.make_async_remote_copy(
            src_ref=message(send, o),
            dst_ref=message(recv, o),
            send_sem=s_send.at[o],
            recv_sem=s_recv.at[o],
            device_id=(offset_device(ep, o, 1), tp),
            device_id_type=MESH,
        )

    def returning(o):
        return pltpu.make_async_remote_copy(
            src_ref=message(back, o),
            dst_ref=message(ret, o),
            send_sem=r_send.at[o],
            recv_sem=r_recv.at[o],
            device_id=(offset_device(ep, o, -1), tp),
            device_id_type=MESH,
        )

    def returning_part(o, n):
        columns = pl.ds(n * (width // PARTS), width // PARTS)
        return pltpu.make_async_remote_copy(
            src_ref=back.at[pl.ds(o * SLABS, SLABS), :, columns],
            dst_ref=ret.at[pl.ds(o * SLABS, SLABS), :, columns],
            send_sem=r_send.at[o + n * per],
            recv_sem=r_recv.at[o + n * per],
            device_id=(offset_device(ep, o, -1), tp),
            device_id_type=MESH,
        )

    own_out = pltpu.make_async_copy(message(send, 0), message(recv, 0), s_recv.at[0])
    own_back = pltpu.make_async_copy(message(back, 0), message(ret, 0), r_recv.at[0])

    def partner_copy(n):
        source, target = weights[n]
        return pltpu.make_async_remote_copy(
            src_ref=source,
            dst_ref=target.at[tp],
            send_sem=w_send.at[n],
            recv_sem=w_recv.at[n],
            device_id=(ep, 1 - tp),
            device_id_type=MESH,
        )

    def chunk_slice(i):
        return pl.ds(pl.multiple_of(i * chunk_slabs, chunk_slabs), chunk_slabs)

    def dispatch(i, carry):
        which = place[pl.ds(pl.multiple_of(i * chunk_rows, chunk_rows), chunk_rows), :]
        for n in range(width // 512):
            columns = slice(n * 512, (n + 1) * 512)
            sent = jnp.dot(which, normed[:, columns], preferred_element_type=jnp.float32)
            send[chunk_slice(i), :, columns] = sent.astype(jnp.bfloat16).reshape(
                chunk_slabs, SLAB, 512
            )

        @pl.when(i == 0)
        def _():
            pl.semaphore_wait(barrier, N_EP)
            own_out.start()

        def go(o, carry):
            outgoing(o).start()
            return carry

        lax.fori_loop(jnp.maximum(i * per, 1), (i + 1) * per, go, 0)

        @pl.when(i == 0)
        def _():
            for n in range(3):
                partner_copy(n).start()

        return carry

    lax.fori_loop(0, chunks, dispatch, 0)

    up0, up1 = upright(target0), upright(target1)
    slot_columns = lax.broadcasted_iota(jnp.int32, (tokens, chunk_rows), 1).astype(jnp.float32)
    for i in range(chunks):
        picks[i, :tokens, :] = jnp.where(slot_columns + float(i * chunk_rows) == up0, 1.0, 0.0).astype(
            jnp.bfloat16
        )
        picks[i, tokens:, :] = jnp.where(slot_columns + float(i * chunk_rows) == up1, 1.0, 0.0).astype(
            jnp.bfloat16
        )
    weight0, weight1 = upright(route[0:1, :]), upright(route[1:2, :])

    for n in range(2):
        pltpu.make_async_copy(weights[n][0], weights[n][1].at[tp], w_load.at[n]).wait()
        partner_copy(n).wait_recv()

    def serve(i, carry):
        def arrive(o, carry):
            outgoing(o).wait_recv()
            return carry

        @pl.when(i == 0)
        def _():
            own_out.wait()

        lax.fori_loop(jnp.maximum(i * per, 1), (i + 1) * per, arrive, 0)
        rows[...] = recv[chunk_slice(i)].reshape(chunk_rows, width)

        for h in range(2):

            def expand(n, carry):
                columns = pl.ds(pl.multiple_of(n * TILE, TILE), TILE)
                gate = jnp.dot(rows[...], wg[h, :, columns], preferred_element_type=jnp.float32)
                up = jnp.dot(rows[...], wu[h, :, columns], preferred_element_type=jnp.float32)
                gate = jnp.minimum(gate, LIMIT)
                up = jnp.clip(up, -LIMIT, LIMIT)
                hidden[h, :, columns] = (
                    (up + 1.0) * gate * jax.nn.sigmoid(ALPHA * gate)
                ).astype(jnp.bfloat16)
                return carry

            lax.fori_loop(0, half // TILE, expand, 0)

        @pl.when(i == 0)
        def _():
            pltpu.make_async_copy(weights[2][0], weights[2][1].at[tp], w_load.at[2]).wait()
            partner_copy(2).wait_recv()

        def contract(n, carry):
            columns = pl.ds(pl.multiple_of(n * 512, 512), 512)
            part0 = jnp.dot(hidden[0], wd[0, :, columns], preferred_element_type=jnp.float32)
            part1 = jnp.dot(hidden[1], wd[1, :, columns], preferred_element_type=jnp.float32)
            both = part0.astype(jnp.bfloat16).astype(jnp.float32) + part1.astype(
                jnp.bfloat16
            ).astype(jnp.float32)
            back[chunk_slice(i), :, columns] = both.astype(jnp.bfloat16).reshape(
                chunk_slabs, SLAB, 512
            )
            return carry

        lax.fori_loop(0, width // 512, contract, 0)

        @pl.when(i == 0)
        def _():
            own_back.start()

        def go(o, carry):
            returning(o).start()
            return carry

        @pl.when(i < chunks - 1)
        def _():
            lax.fori_loop(jnp.maximum(i * per, 1), (i + 1) * per, go, 0)

        @pl.when(i == chunks - 1)
        def _():
            for n in range(PARTS):

                def go_part(o, carry):
                    returning_part(o, n).start()
                    return carry

                lax.fori_loop(N_EP - per, N_EP, go_part, 0)

        return carry

    lax.fori_loop(0, chunks, serve, 0)

    def sent(o, carry):
        outgoing(o).wait_send()
        return carry

    lax.fori_loop(1, N_EP, sent, 0)
    for n in range(3):
        partner_copy(n).wait_send()

    def mixed(i, n):
        came = ret[chunk_slice(i), :, n * 512 : (n + 1) * 512].reshape(chunk_rows, 512)
        both = jnp.dot(picks[i], came, preferred_element_type=jnp.float32)
        return (
            both[:tokens] * weight0 + both[tokens:] * weight1
        )

    def collect(i, carry):
        def arrive(o, carry):
            returning(o).wait_send()
            returning(o).wait_recv()
            return carry

        @pl.when(i == 0)
        def _():
            own_back.wait()

        lax.fori_loop(jnp.maximum(i * per, 1), (i + 1) * per, arrive, 0)
        for n in range(width // 512):
            mine = mixed(i, n)
            columns = slice(n * 512, (n + 1) * 512)

            @pl.when(i == 0)
            def _():
                total[:, columns] = mine

            @pl.when(i > 0)
            def _():
                total[:, columns] += mine

        return carry

    lax.fori_loop(0, chunks - 1, collect, 0)

    post_gain = post_ref[...]
    squares = jnp.zeros((tokens, 1), jnp.float32)
    last = chunks - 1
    for h in range(PARTS):

        def arrive_part(o, carry):
            returning_part(o, h).wait_send()
            returning_part(o, h).wait_recv()
            return carry

        lax.fori_loop(last * per, N_EP, arrive_part, 0)
        for n in range(h * width // 512 // PARTS, (h + 1) * width // 512 // PARTS):
            columns = slice(n * 512, (n + 1) * 512)
            part = total[:, columns] + mixed(last, n)
            total[:, columns] = part
            squares += jnp.sum(part * part, axis=1, keepdims=True)
    scale = lax.rsqrt(squares / float(width) + EPSILON)
    for n in range(width // 512):
        columns = slice(n * 512, (n + 1) * 512)
        out_ref[:, columns] = (total[:, columns] * scale * post_gain[:, columns]).astype(jnp.bfloat16)


def local(inputs, pre_gain, expert_ids, route_weights, gate_proj, up_proj, down_proj, post_gain):
    tokens, width = inputs.shape
    half = gate_proj.shape[2]
    chunks = 4
    chunk_rows = N_EP // chunks * CAP
    slabs = N_EP * SLABS
    bf16, f32 = jnp.bfloat16, jnp.float32
    vmem = pl.BlockSpec(memory_space=pltpu.VMEM)
    hbm = pl.BlockSpec(memory_space=pl.ANY)
    dma = pltpu.SemaphoreType.DMA
    return pl.pallas_call(
        functools.partial(kernel, chunks),
        out_shape=pltpu.VMEM((tokens, width), bf16),
        in_specs=[hbm, vmem, vmem, vmem, hbm, hbm, hbm, vmem],
        out_specs=vmem,
        scratch_shapes=[
            pltpu.VMEM((tokens, width), bf16),
            pltpu.VMEM((tokens, width), bf16),
            pltpu.VMEM((N_EP * CAP, tokens), bf16),
            pltpu.VMEM((chunks, 2 * tokens, chunk_rows), bf16),
            pltpu.VMEM((slabs, SLAB, width), bf16),
            pltpu.VMEM((slabs, SLAB, width), bf16),
            pltpu.VMEM((2, width, half), bf16),
            pltpu.VMEM((2, width, half), bf16),
            pltpu.VMEM((2, half, width), bf16),
            pltpu.VMEM((chunk_rows, width), bf16),
            pltpu.VMEM((2, chunk_rows, half), bf16),
            pltpu.VMEM((slabs, SLAB, width), bf16),
            pltpu.VMEM((slabs, SLAB, width), bf16),
            pltpu.VMEM((tokens, width), f32),
            dma,
            dma((3,)),
            dma((3,)),
            dma((3,)),
            dma((N_EP,)),
            dma((N_EP,)),
            dma((N_EP + (PARTS - 1) * N_EP // chunks,)),
            dma((N_EP + (PARTS - 1) * N_EP // chunks,)),
        ],
        compiler_params=pltpu.CompilerParams(
            collective_id=0, has_side_effects=True, vmem_limit_bytes=60 * 1024 * 1024
        ),
    )(
        inputs,
        pre_gain.reshape(1, width),
        expert_ids.T,
        route_weights.T,
        gate_proj[0],
        up_proj[0],
        down_proj[0],
        post_gain.reshape(1, width),
    )


def solution(mesh):
    in_specs = (
        P(("ep", "tp"), None),
        P(),
        P(("ep", "tp"), None),
        P(("ep", "tp"), None),
        P("ep", None, "tp"),
        P("ep", None, "tp"),
        P("ep", "tp", None),
        P(),
    )
    out_specs = P(("ep", "tp"), None)
    return jax.shard_map(local, mesh=mesh, in_specs=in_specs, out_specs=out_specs, check_vma=False)
```
